32 devices in a mesh: sp: 16 (over z, y, x), tp: 2 (over core).
Axes of the slice: x: 2, y: 2, z: 4, core: 2. Of those that a mesh axis runs over, the one named last changes fastest.
Arguments:
- features: bfloat16 [4096, 1024], P('sp', 'tp'), may hold values from -6 to 6
- lambda_real: float32 [64, 64], P('tp'), may hold values from -4 to 0, as said below
- lambda_imag: float32 [64, 64], P('tp'), may hold values from 0.5 to 201.06177
- log_step: float32 [64], P('tp'), may hold values from -5 to -2
- input_real: float32 [64, 64, 16], P('tp'), may hold values from -2 to 2
- input_imag: float32 [64, 64, 16], P('tp'), may hold values from -2 to 2
- real_output: float32 [64, 16, 64], P('tp'), may hold values from -0.75 to 0.75
- imaginary_output: float32 [64, 16, 64], P('tp'), may hold values from -0.75 to 0.75
- skip_gain: float32 [1024], P('tp'), may hold values from -4 to 4
- value_weight: bfloat16 [1024, 2048], P('tp'), may hold values from -0.1875 to 0.1875
- gate_weight: bfloat16 [1024, 2048], P('tp'), may hold values from -0.1875 to 0.1875
- value_bias: float32 [2048], replicated, may hold values from -3 to 3
- gate_bias: float32 [2048], replicated, may hold values from -3 to 3
Outputs:
- mixed_output: bfloat16 [4096, 2048], P(('sp', 'tp'))
The draws below stay inside these ranges and needn't reach their ends.
Inputs may be any that keep to these rules, and one draw needn't show every extreme that they name: `lambda_real`: negative.
All inputs are finite; a program needn't handle non-finite values.
Results may differ from the reference program's by a relative error of at most 0.03.
Values may be sent and summed in bfloat16 or wider, within the bound.
A program may use at most 128 MiB of HBM per device.

```python
import math
import jax
import jax.numpy as jnp
from jax import lax

D = 2048
CHANNELS = 1024
GROUP = 16
STATE = 64
TOK_SP = 256
GROUPS = 64
LENGTH = 4096
N_TP = 2


def group_rates(key):
    base_key = jax.random.fold_in(key, 91)
    key_flag, key_step, key_rate = jax.random.split(base_key, 3)
    fast_share = 5
    fast_flag = jax.random.randint(key_flag, (GROUPS,), 0, 10) < fast_share
    log_step = jax.random.uniform(key_step, (GROUPS,), jnp.float32, math.log(0.01), math.log(0.1))
    step_size = jnp.exp(log_step)[:, None]
    rate_draw = jax.random.uniform(key_rate, (GROUPS, STATE), jnp.float32, 0.0, 1.0)
    fast_rate = (0.01 + 0.023 * rate_draw) / step_size
    slow_rate = (0.3 + 1.7 * rate_draw) / (LENGTH * step_size)
    lambda_real = -jnp.where(fast_flag[:, None], fast_rate, slow_rate)
    return (lambda_real.astype(jnp.float32), log_step.astype(jnp.float32))


def draw_lambda_real(key, part):
    return group_rates(key)[0]


def draw_log_step(key, part):
    return group_rates(key)[1]


def block_levels(key, dims, cuts, low, top_value):
    loudness = 1.0
    for dim, blocks in cuts:
        draws = jax.random.uniform(jax.random.fold_in(jax.random.fold_in(key, 6), dim), (blocks,), jnp.float32, low / len(cuts), top_value / len(cuts))
        loudness = loudness * jnp.repeat(jnp.exp(draws), dims[dim] // blocks).reshape((-1,) + (1,) * (len(dims) - 1 - dim))
    return loudness


def normal_values(own_key, extent, width, bound, pieces=(), held_as=jnp.bfloat16):
    values = jax.random.normal(own_key, extent, jnp.float32) * width
    if len(pieces) > 0:
        values = block_levels(own_key, extent, pieces, -0.22, 0.18) * values
    return jnp.clip(values, min=-bound, max=bound).astype(held_as)


def setup_inputs(seed: int = 0) -> dict:
    splits = jax.random.split(jax.random.key(seed), 14)
    return {
        "features": normal_values(splits[0], (LENGTH, CHANNELS), 1.0, 6.0, ((0, 16), (1, 2))),
        "lambda_real": draw_lambda_real(jax.random.fold_in(splits[13], 71), 0),
        "lambda_imag": jnp.clip(0.5 + 200.56177 * jax.random.uniform(splits[2], (GROUPS, STATE), jnp.float32) ** block_levels(splits[2], (GROUPS, STATE), ((0, 2),), -0.2, 0.2), 0.5, 201.06177),
        "log_step": draw_log_step(jax.random.fold_in(splits[13], 71), 0),
        "input_real": normal_values(splits[4], (GROUPS, STATE, GROUP), (max(4, LENGTH // 512)) ** -0.5, 2.0, ((0, 2),), jnp.float32),
        "input_imag": normal_values(splits[5], (GROUPS, STATE, GROUP), (max(4, LENGTH // 512)) ** -0.5, 2.0, ((0, 2),), jnp.float32),
        "real_output": normal_values(splits[6], (GROUPS, GROUP, STATE), STATE ** -0.5, 0.75, ((0, 2),), jnp.float32),
        "imaginary_output": normal_values(splits[7], (GROUPS, GROUP, STATE), STATE ** -0.5, 0.75, ((0, 2),), jnp.float32),
        "skip_gain": normal_values(splits[8], (CHANNELS,), 1.0, 4.0, ((0, 2),), jnp.float32),
        "value_weight": normal_values(splits[9], (CHANNELS, D), CHANNELS ** -0.5, 0.1875, ((0, 2),)),
        "gate_weight": normal_values(splits[10], (CHANNELS, D), CHANNELS ** -0.5, 0.1875, ((0, 2),)),
        "value_bias": normal_values(splits[11], (D,), 0.5, 3.0, (), jnp.float32),
        "gate_bias": normal_values(splits[12], (D,), 0.5, 3.0, (), jnp.float32),
    }


def discretize(lambda_real, lambda_imag, log_step, input_real, input_imag):
    step_size = jnp.exp(log_step)[:, None]
    magnitude = jnp.exp(lambda_real * step_size)
    phase_arg = lambda_imag * step_size
    trans_re = magnitude * jnp.cos(phase_arg)
    trans_im = magnitude * jnp.sin(phase_arg)
    denominator = lambda_real * lambda_real + lambda_imag * lambda_imag
    num_re = trans_re - 1.0
    num_im = trans_im
    f_re = (num_re * lambda_real + num_im * lambda_imag) / denominator
    f_im = (num_im * lambda_real - num_re * lambda_imag) / denominator
    bar_re = f_re[..., None] * input_real - f_im[..., None] * input_imag
    bar_im = f_re[..., None] * input_imag + f_im[..., None] * input_real
    return step_size, bar_re, bar_im


def powers(lambda_real, lambda_imag, step_size, positions):
    exponent = (jnp.arange(positions, dtype=jnp.int32) + 1).astype(jnp.float32)[:, None, None]
    magnitude = jnp.exp(exponent * lambda_real * step_size)
    phase_arg = exponent * lambda_imag * step_size
    return magnitude * jnp.cos(phase_arg), magnitude * jnp.sin(phase_arg)


def combine(earlier, later):
    a1r, a1i, b1r, b1i = earlier
    a2r, a2i, b2r, b2i = later
    return (a1r * a2r - a1i * a2i, a1r * a2i + a1i * a2r,
            a2r * b1r - a2i * b1i + b2r, a2r * b1i + a2i * b1r + b2i)


def local_states(trans_re, trans_im, bu_re, bu_im):
    a_re = jnp.broadcast_to(trans_re, bu_re.shape)
    a_im = jnp.broadcast_to(trans_im, bu_im.shape)
    result = lax.associative_scan(combine, (a_re, a_im, bu_re, bu_im), axis=0)
    return result[2], result[3]


def reference(features, lambda_real, lambda_imag, log_step, input_real, input_imag, real_output,
              imaginary_output, skip_gain, value_weight, gate_weight, value_bias, gate_bias):
    upper_limit = lax.Precision.HIGHEST
    step_size, bar_re, bar_im = discretize(lambda_real, lambda_imag, log_step, input_real, input_imag)
    pw_re, pw_im = powers(lambda_real, lambda_imag, step_size, TOK_SP)
    blocks = features.reshape(LENGTH // TOK_SP, TOK_SP, CHANNELS)
    slice_width = CHANNELS // N_TP

    def partials(activated, weight):
        total = jnp.zeros((TOK_SP, D), jnp.float32)
        for index in range(N_TP):
            left = activated[:, index * slice_width:(index + 1) * slice_width]
            right = weight[index * slice_width:(index + 1) * slice_width]
            rounded = lax.optimization_barrier(jnp.dot(left, right, preferred_element_type=jnp.float32).astype(jnp.bfloat16))
            total = total + rounded.astype(jnp.float32)
        return total

    def advance(carried, rows_per_block):
        h_re, h_im = carried
        widened = rows_per_block.astype(jnp.float32)
        grouped = widened.reshape(TOK_SP, GROUPS, GROUP)
        bu_re = jnp.einsum('sgc,gpc->sgp', grouped, bar_re, precision=upper_limit)
        bu_im = jnp.einsum('sgc,gpc->sgp', grouped, bar_im, precision=upper_limit)
        signal_real, signal_imaginary = local_states(pw_re[0], pw_im[0], bu_re, bu_im)
        signal_real = signal_real + pw_re * h_re - pw_im * h_im
        signal_imaginary = signal_imaginary + pw_re * h_im + pw_im * h_re
        mixer_response = (jnp.einsum('qej,eoj->qeo', signal_real, real_output, precision=upper_limit)
                    - jnp.einsum('qej,eoj->qeo', signal_imaginary, imaginary_output, precision=upper_limit))
        mixer_response = mixer_response.reshape(TOK_SP, CHANNELS) + skip_gain * widened
        activated = jax.nn.gelu(mixer_response).astype(jnp.bfloat16)
        value_sum = partials(activated, value_weight) + value_bias
        gate_sum = partials(activated, gate_weight) + gate_bias
        result = (value_sum * jax.nn.sigmoid(gate_sum)).astype(jnp.bfloat16)
        return (signal_real[-1], signal_imaginary[-1]), result

    start_state = (jnp.zeros((GROUPS, STATE), jnp.float32), jnp.zeros((GROUPS, STATE), jnp.float32))
    _, outputs = lax.scan(advance, start_state, blocks)
    return outputs.reshape(LENGTH, D)
```

```python
import functools

import jax
import jax.numpy as jnp
from jax import lax
from jax.experimental import pallas as pl
from jax.experimental.pallas import tpu as pltpu
from jax.sharding import PartitionSpec as P

MESH = pl.DeviceIdType.MESH
F32 = jnp.float32
BF16 = jnp.bfloat16


def iota(shape, dim):
    return lax.broadcasted_iota(jnp.int32, shape, dim)


def cmul(ar, ai, br, bi):
    return ar * br - ai * bi, ar * bi + ai * br


def nt_dot(left, right):
    return lax.dot_general(left, right, (((1,), (1,)), ((), ())), preferred_element_type=F32)


def kernel(nsp, ntp, dims, *refs):
    rows, groups, state, size, width = dims
    (x_h, lr_h, li_h, ls_h, br_h, bi_h, cr_h, ci_h, sk_h, vw_h, gw_h, vb_h, gb_h, out_ref,
     x_v, lr_v, li_v, ls_v, br_v, bi_v, cr_v, ci_v, sk_v, vw_v, gw_v, vb_v, gb_v,
     xp_v, zr_v, zi_v, zcat_v, wcat_v, crm_v, cim_v, resp_v, act_v,
     hx_v, fin_v, a_all_v, msg_v, recv_v, h_v, part_v, inbox_v,
     in_sem, send_sem, recv_sem, psend_sem, precv_sem) = refs
    me = lax.axis_index("sp")
    core = lax.axis_index("tp")
    gpb = 128 // size
    lanes = gpb * state
    blocks = groups // gpb
    chunks = 16
    length = rows // chunks
    own_rows = rows // ntp

    hbm = (ls_h, lr_h, li_h, x_h, br_h, bi_h, cr_h, ci_h, sk_h, vb_h, gb_h, vw_h, gw_h)
    vmem = (ls_v, lr_v, li_v, x_v, br_v, bi_v, cr_v, ci_v, sk_v, vb_v, gb_v, vw_v, gw_v)
    copies = [pltpu.make_async_copy(s, d, in_sem.at[i]) for i, (s, d) in enumerate(zip(hbm, vmem))]
    for c in copies:
        c.start()

    barrier = pltpu.get_barrier_semaphore()
    for k in range(1, ntp):
        pl.semaphore_signal(barrier, inc=1, device_id=(me, lax.rem(core + k, ntp)), device_id_type=MESH)

    @pl.loop(1, nsp)
    def _(k):
        pl.semaphore_signal(barrier, inc=1, device_id=(lax.rem(me + k, nsp), core), device_id_type=MESH)

    for c in copies[:3]:
        c.wait()
    eye = iota((groups, groups), 0) == iota((groups, groups), 1)
    step = jnp.exp(jnp.sum(jnp.where(eye, ls_v[...], 0.0), axis=1, keepdims=True))
    lam_r, lam_i = lr_v[...], li_v[...]
    mag = jnp.exp(lam_r * step)
    phase = lam_i * step
    t_r, t_i = mag * jnp.cos(phase), mag * jnp.sin(phase)
    den = lam_r * lam_r + lam_i * lam_i
    n_r = t_r - 1.0
    f_r = (n_r * lam_r + t_i * lam_i) / den
    f_i = (t_i * lam_r - n_r * lam_i) / den

    per = 128 // state
    row8, lane8 = iota((gpb, 128), 0), iota((gpb, 128), 1)

    def flat(value, b):
        sub = value[b * gpb:(b + 1) * gpb]
        dup = jnp.concatenate([sub] * per, axis=1)
        return jnp.concatenate(
            [jnp.sum(jnp.where(row8 == per * j + lane8 // state, dup, 0.0), axis=0, keepdims=True)
             for j in range(gpb // per)], axis=1)

    r0, r1 = iota((rows, rows), 0), iota((rows, rows), 1)
    shuffle = jnp.where(r1 == (r0 % chunks) * length + r0 // chunks, 1.0, 0.0).astype(BF16)
    copies[3].wait()
    xp_v[...] = jnp.dot(shuffle, x_v[...], preferred_element_type=F32).astype(BF16)

    spread = jnp.where(iota((size, 128), 1) % size == iota((size, 128), 0), 1.0, 0.0).astype(BF16)
    b_mask = iota((lanes, 128), 0) // state == iota((lanes, 128), 1) // size
    copies[4].wait()
    copies[5].wait()
    crow = iota((chunks, lanes), 0)

    def shift(value, s):
        return jnp.where(crow >= s, pltpu.roll(value, s, 0), 0.0)

    powers = []
    for b in range(blocks):
        xb = xp_v[:, b * 128:(b + 1) * 128]

        def inject(ref):
            flat_b = ref[b * gpb:(b + 1) * gpb].reshape(lanes, size).astype(BF16)
            wide = jnp.dot(flat_b, spread, preferred_element_type=F32)
            return nt_dot(xb, jnp.where(b_mask, wide, 0.0).astype(BF16))

        zr_v[b] = inject(br_v)
        zi_v[b] = inject(bi_v)
        a1r, a1i = flat(t_r, b), flat(t_i, b)
        ar, ai = jnp.broadcast_to(a1r, (chunks, lanes)), jnp.broadcast_to(a1i, (chunks, lanes))
        z_r = z_i = None
        for o in range(length):
            here = pl.ds(o * chunks, chunks)
            if o == 0:
                z_r, z_i = zr_v[b, here, :], zi_v[b, here, :]
            else:
                p_r, p_i = cmul(ar, ai, z_r, z_i)
                z_r, z_i = p_r + zr_v[b, here, :], p_i + zi_v[b, here, :]
                zr_v[b, here, :] = z_r
                zi_v[b, here, :] = z_i
        qr, qi = ar, ai
        s = 1
        while s < length:
            qr, qi = cmul(qr, qi, qr, qi)
            s *= 2
        pw_r, pw_i = jnp.ones_like(qr), jnp.zeros_like(qr)
        s = 1
        while s < chunks:
            m_r, m_i = cmul(qr, qi, shift(z_r, s), shift(z_i, s))
            z_r, z_i = z_r + m_r, z_i + m_i
            bit = (crow // s) % 2 == 1
            pw_r, pw_i = cmul(pw_r, pw_i, jnp.where(bit, qr, 1.0), jnp.where(bit, qi, 0.0))
            qr, qi = cmul(qr, qi, qr, qi)
            s *= 2
        hx_v[0, b], hx_v[1, b] = shift(z_r, 1), shift(z_i, 1)
        fin_v[b:b + 1] = z_r[chunks - 1:]
        fin_v[blocks + b:blocks + b + 1] = z_i[chunks - 1:]
        a_all_v[b:b + 1] = qr[:1]
        a_all_v[blocks + b:blocks + b + 1] = qi[:1]
        hx_v[2, b], hx_v[3, b] = pw_r, pw_i
    msg_v[...] = fin_v[...].astype(BF16)

    pl.semaphore_wait(barrier, nsp - 1 + ntp - 1)

    def outgoing(d):
        return pltpu.make_async_remote_copy(
            src_ref=msg_v, dst_ref=recv_v.at[me], send_sem=send_sem.at[d], recv_sem=recv_sem.at[me],
            device_id=(d, core), device_id_type=MESH)

    @pl.loop(me + 1, nsp)
    def _(d):
        outgoing(nsp + me - d).start()

    copies[6].wait()
    copies[7].wait()
    copies[8].wait()
    c_mask = iota((128, lanes), 0) // size == iota((128, lanes), 1) // state
    for b in range(blocks):
        a1r, a1i = flat(t_r, b), flat(t_i, b)
        ar, ai = jnp.broadcast_to(a1r, (chunks, lanes)), jnp.broadcast_to(a1i, (chunks, lanes))
        w_r, w_i = hx_v[0, b], hx_v[1, b]
        p_r, p_i = hx_v[2, b], hx_v[3, b]
        for o in range(length):
            here = pl.ds(o * chunks, chunks)
            w_r, w_i = cmul(ar, ai, w_r, w_i)
            p_r, p_i = cmul(ar, ai, p_r, p_i)
            zcat_v[here, :lanes] = (zr_v[b, here, :] + w_r).astype(BF16)
            zcat_v[here, lanes:] = (zi_v[b, here, :] + w_i).astype(BF16)
            wcat_v[b, here, :lanes] = p_r.astype(BF16)
            wcat_v[b, here, lanes:] = p_i.astype(BF16)
        gains_r, gains_i = [], []
        for g in range(b * gpb, (b + 1) * gpb):
            g_r, g_i = cmul(cr_v[g], ci_v[g], f_r[g:g + 1], f_i[g:g + 1])
            gains_r.append(g_r)
            gains_i.append(g_i)

        def diagonal(parts):
            tall = jnp.concatenate(parts, axis=0)
            wide = jnp.concatenate([tall] * gpb, axis=1)
            return jnp.where(c_mask, wide, 0.0)

        m_r, m_i = diagonal(gains_r), diagonal(gains_i)
        crm_v[b], cim_v[b] = m_r, m_i
        mats = jnp.concatenate([m_r.astype(BF16), (-m_i).astype(BF16)], axis=1)
        col = pl.ds(b * 128, 128)
        resp_v[:, col] = nt_dot(zcat_v[...], mats) + sk_v[:, col] * xp_v[:, col].astype(F32)

    A_r, A_i = a_all_v[:blocks], a_all_v[blocks:]
    zero = jnp.zeros((blocks, lanes), F32)

    def horner(d, h):
        pltpu.make_async_remote_copy(
            src_ref=msg_v, dst_ref=recv_v.at[d], send_sem=send_sem.at[d], recv_sem=recv_sem.at[d],
            device_id=(d, core), device_id_type=MESH).wait_recv()
        got = recv_v[d].astype(F32)
        n_r, n_i = cmul(A_r, A_i, h[0], h[1])
        return n_r + got[:blocks], n_i + got[blocks:]

    h_r, h_i = lax.fori_loop(0, me, horner, (zero, zero))
    h_v[:blocks] = h_r
    h_v[blocks:] = h_i

    for b in range(blocks):
        k_r, k_i = cmul(crm_v[b], cim_v[b], h_v[b:b + 1], h_v[blocks + b:blocks + b + 1])
        mats = jnp.concatenate([k_r.astype(BF16), (-k_i).astype(BF16)], axis=1)
        col = pl.ds(b * 128, 128)
        total = resp_v[:, col] + nt_dot(wcat_v[b], mats)
        act_v[:, col] = jax.nn.gelu(total).astype(BF16)

    back = jnp.where(r1 == (r0 % length) * chunks + r0 // length, 1.0, 0.0).astype(BF16)
    act = jnp.dot(back, act_v[...], preferred_element_type=F32).astype(BF16)

    for c in copies[9:]:
        c.wait()
    piece = inbox_v.shape[-1]
    pieces = width // piece

    def exchange(j, k):
        to = lax.rem(core + k, ntp)
        return pltpu.make_async_remote_copy(
            src_ref=part_v.at[j, to], dst_ref=inbox_v.at[j, k - 1],
            send_sem=psend_sem.at[j, k - 1], recv_sem=precv_sem.at[j, k - 1],
            device_id=(me, to), device_id_type=MESH)

    for j in range(pieces):
        col = pl.ds(j * piece, piece)
        for which, weight in enumerate((vw_v, gw_v)):
            part = jnp.dot(act, weight[:, col], preferred_element_type=F32).astype(BF16)
            for i in range(ntp):
                part_v[j, i, which] = part[i * own_rows:(i + 1) * own_rows]
        for k in range(1, ntp):
            exchange(j, k).start()
    for j in range(pieces):
        col = pl.ds(j * piece, piece)
        for k in range(1, ntp):
            exchange(j, k).wait_recv()
        sums = []
        for which, bias in enumerate((vb_v, gb_v)):
            total = part_v[j, core, which].astype(F32)
            for k in range(1, ntp):
                total = total + inbox_v[j, k - 1, which].astype(F32)
            sums.append(total + bias[:, col])
        out_ref[:, col] = (sums[0] * jax.nn.sigmoid(sums[1])).astype(BF16)
    for j in range(pieces):
        for k in range(1, ntp):
            exchange(j, k).wait_send()

    @pl.loop(me + 1, nsp)
    def _(d):
        outgoing(nsp + me - d).wait_send()


def local(nsp, ntp, features, lambda_real, lambda_imag, log_step, input_real, input_imag, real_output,
          imaginary_output, skip_gain, value_weight, gate_weight, value_bias, gate_bias):
    rows, channels = features.shape
    groups, state = lambda_real.shape
    size = input_real.shape[2]
    width = value_weight.shape[1]
    gpb = 128 // size
    lanes, blocks, chunks = gpb * state, groups // gpb, 16
    piece = min(512, width)
    args = (features, lambda_real, lambda_imag, log_step[None], input_real, input_imag, real_output,
            imaginary_output, skip_gain[None], value_weight, gate_weight, value_bias[None], gate_bias[None])
    scratch = [pltpu.VMEM(a.shape, a.dtype) for a in args]
    scratch += [
        pltpu.VMEM((rows, channels), BF16),
        pltpu.VMEM((blocks, rows, lanes), F32),
        pltpu.VMEM((blocks, rows, lanes), F32),
        pltpu.VMEM((rows, 2 * lanes), BF16),
        pltpu.VMEM((blocks, rows, 2 * lanes), BF16),
        pltpu.VMEM((blocks, 128, lanes), F32),
        pltpu.VMEM((blocks, 128, lanes), F32),
        pltpu.VMEM((rows, channels), F32),
        pltpu.VMEM((rows, channels), BF16),
        pltpu.VMEM((4, blocks, chunks, lanes), F32),
        pltpu.VMEM((2 * blocks, lanes), F32),
        pltpu.VMEM((2 * blocks, lanes), F32),
        pltpu.VMEM((2 * blocks, lanes), BF16),
        pltpu.VMEM((nsp, 2 * blocks, lanes), BF16),
        pltpu.VMEM((2 * blocks, lanes), F32),
        pltpu.VMEM((width // piece, ntp, 2, rows // ntp, piece), BF16),
        pltpu.VMEM((width // piece, ntp - 1, 2, rows // ntp, piece), BF16),
        pltpu.SemaphoreType.DMA((len(args),)),
        pltpu.SemaphoreType.DMA((nsp,)),
        pltpu.SemaphoreType.DMA((nsp,)),
        pltpu.SemaphoreType.DMA((width // piece, ntp - 1)),
        pltpu.SemaphoreType.DMA((width // piece, ntp - 1)),
    ]
    return pl.pallas_call(
        functools.partial(kernel, nsp, ntp, (rows, groups, state, size, width)),
        out_shape=jax.ShapeDtypeStruct((rows // ntp, width), BF16),
        in_specs=[pl.BlockSpec(memory_space=pl.ANY)] * len(args),
        out_specs=pl.BlockSpec(memory_space=pltpu.VMEM),
        scratch_shapes=scratch,
        compiler_params=pltpu.CompilerParams(
            collective_id=0, has_side_effects=True, vmem_limit_bytes=60 * 1024 * 1024),
        name="mixer",
    )(*args)


def solution(mesh):
    in_specs = (
        P("sp", "tp"),
        P("tp", None),
        P("tp", None),
        P("tp"),
        P("tp", None, None),
        P("tp", None, None),
        P("tp", None, None),
        P("tp", None, None),
        P("tp"),
        P("tp", None),
        P("tp", None),
        P(),
        P(),
    )
    out_specs = P(("sp", "tp"), None)
    body = functools.partial(local, mesh.shape["sp"], mesh.shape["tp"])
    return jax.shard_map(body, mesh=mesh, in_specs=in_specs, out_specs=out_specs, check_vma=False)
```

```python
import functools

import jax
import jax.numpy as jnp
from jax import lax
from jax.experimental import pallas as pl
from jax.experimental.pallas import tpu as pltpu
from jax.sharding import PartitionSpec as P

MESH = pl.DeviceIdType.MESH
F32 = jnp.float32
BF16 = jnp.bfloat16


def iota(shape, dim):
    return lax.broadcasted_iota(jnp.int32, shape, dim)


def cmul(ar, ai, br, bi):
    return ar * br - ai * bi, ar * bi + ai * br


def nt_dot(left, right):
    return lax.dot_general(left, right, (((1,), (1,)), ((), ())), preferred_element_type=F32)


def kernel(nsp, ntp, dims, *refs):
    rows, groups, state, size, width = dims
    (x_h, lr_h, li_h, ls_h, br_h, bi_h, cr_h, ci_h, sk_h, vw_h, gw_h, vb_h, gb_h, out_ref,
     x_v, lr_v, li_v, ls_v, br_v, bi_v, cr_v, ci_v, sk_v, vw_v, gw_v, vb_v, gb_v,
     xp_v, zr_v, zi_v, zcat_v, wcat_v, crm_v, cim_v, resp_v, act_v,
     hx_v, fin_v, a_all_v, msg_v, recv_v, h_v, part_v, inbox_v,
     in_sem, send_sem, recv_sem, psend_sem, precv_sem) = refs
    me = lax.axis_index("sp")
    core = lax.axis_index("tp")
    gpb = 128 // size
    lanes = gpb * state
    blocks = groups // gpb
    chunks = 16
    length = rows // chunks
    own_rows = rows // ntp

    hbm = (ls_h, lr_h, li_h, x_h, br_h, bi_h, cr_h, ci_h, sk_h, vb_h, gb_h, vw_h, gw_h)
    vmem = (ls_v, lr_v, li_v, x_v, br_v, bi_v, cr_v, ci_v, sk_v, vb_v, gb_v, vw_v, gw_v)
    copies = [pltpu.make_async_copy(s, d, in_sem.at[i]) for i, (s, d) in enumerate(zip(hbm, vmem))]
    for c in copies:
        c.start()

    barrier = pltpu.get_barrier_semaphore()
    for k in range(1, ntp):
        pl.semaphore_signal(barrier, inc=1, device_id=(me, lax.rem(core + k, ntp)), device_id_type=MESH)

    @pl.loop(1, nsp)
    def _(k):
        pl.semaphore_signal(barrier, inc=1, device_id=(lax.rem(me + k, nsp), core), device_id_type=MESH)

    for c in copies[:3]:
        c.wait()
    eye = iota((groups, groups), 0) == iota((groups, groups), 1)
    step = jnp.exp(jnp.sum(jnp.where(eye, ls_v[...], 0.0), axis=1, keepdims=True))
    lam_r, lam_i = lr_v[...], li_v[...]
    mag = jnp.exp(lam_r * step)
    phase = lam_i * step
    t_r, t_i = mag * jnp.cos(phase), mag * jnp.sin(phase)
    den = lam_r * lam_r + lam_i * lam_i
    n_r = t_r - 1.0
    f_r = (n_r * lam_r + t_i * lam_i) / den
    f_i = (t_i * lam_r - n_r * lam_i) / den

    per = 128 // state
    row8, lane8 = iota((gpb, 128), 0), iota((gpb, 128), 1)

    def flat(value, b):
        sub = value[b * gpb:(b + 1) * gpb]
        dup = jnp.concatenate([sub] * per, axis=1)
        return jnp.concatenate(
            [jnp.sum(jnp.where(row8 == per * j + lane8 // state, dup, 0.0), axis=0, keepdims=True)
             for j in range(gpb // per)], axis=1)

    r0, r1 = iota((rows, rows), 0), iota((rows, rows), 1)
    shuffle = jnp.where(r1 == (r0 % chunks) * length + r0 // chunks, 1.0, 0.0).astype(BF16)
    copies[3].wait()
    xp_v[...] = jnp.dot(shuffle, x_v[...], preferred_element_type=F32).astype(BF16)


    c_mask = iota((128, lanes), 0) // size == iota((128, lanes), 1) // state

    def diagonal(tall):
        return jnp.where(c_mask, jnp.concatenate([tall] * gpb, axis=1), 0.0)

    copies[4].wait()
    copies[5].wait()
    crow = iota((chunks, lanes), 0)

    def shift(value, s):
        return jnp.where(crow >= s, pltpu.roll(value, s, 0), 0.0)

    for b in range(blocks):
        xb = xp_v[:, b * 128:(b + 1) * 128]

        def inject(ref):
            mat = diagonal(ref[b * gpb:(b + 1) * gpb].reshape(128, state)).astype(BF16)
            return jnp.dot(xb, mat, preferred_element_type=F32)

        zr_v[b] = inject(br_v)
        zi_v[b] = inject(bi_v)
        a1r, a1i = flat(t_r, b), flat(t_i, b)
        ar, ai = jnp.broadcast_to(a1r, (chunks, lanes)), jnp.broadcast_to(a1i, (chunks, lanes))
        z_r = z_i = None
        for o in range(length):
            here = pl.ds(o * chunks, chunks)
            if o == 0:
                z_r, z_i = zr_v[b, here, :], zi_v[b, here, :]
            else:
                p_r, p_i = cmul(ar, ai, z_r, z_i)
                z_r, z_i = p_r + zr_v[b, here, :], p_i + zi_v[b, here, :]
                zr_v[b, here, :] = z_r
                zi_v[b, here, :] = z_i
        qr, qi = ar, ai
        s = 1
        while s < length:
            qr, qi = cmul(qr, qi, qr, qi)
            s *= 2
        pw_r, pw_i = jnp.ones_like(qr), jnp.zeros_like(qr)
        s = 1
        while s < chunks:
            m_r, m_i = cmul(qr, qi, shift(z_r, s), shift(z_i, s))
            z_r, z_i = z_r + m_r, z_i + m_i
            bit = (crow // s) % 2 == 1
            pw_r, pw_i = cmul(pw_r, pw_i, jnp.where(bit, qr, 1.0), jnp.where(bit, qi, 0.0))
            qr, qi = cmul(qr, qi, qr, qi)
            s *= 2
        hx_v[0, b], hx_v[1, b] = shift(z_r, 1), shift(z_i, 1)
        fin_v[b:b + 1] = z_r[chunks - 1:]
        fin_v[blocks + b:blocks + b + 1] = z_i[chunks - 1:]
        a_all_v[b:b + 1] = qr[:1]
        a_all_v[blocks + b:blocks + b + 1] = qi[:1]
        hx_v[2, b], hx_v[3, b] = pw_r, pw_i
    msg_v[...] = fin_v[...].astype(BF16)

    pl.semaphore_wait(barrier, nsp - 1 + ntp - 1)

    def outgoing(d):
        return pltpu.make_async_remote_copy(
            src_ref=msg_v, dst_ref=recv_v.at[me], send_sem=send_sem.at[d], recv_sem=recv_sem.at[me],
            device_id=(d, core), device_id_type=MESH)

    @pl.loop(me + 1, nsp)
    def _(d):
        outgoing(nsp + me - d).start()

    copies[6].wait()
    copies[7].wait()
    copies[8].wait()
    for b in range(blocks):
        a1r, a1i = flat(t_r, b), flat(t_i, b)
        ar, ai = jnp.broadcast_to(a1r, (chunks, lanes)), jnp.broadcast_to(a1i, (chunks, lanes))
        w_r, w_i = hx_v[0, b], hx_v[1, b]
        p_r, p_i = hx_v[2, b], hx_v[3, b]
        for o in range(length):
            here = pl.ds(o * chunks, chunks)
            w_r, w_i = cmul(ar, ai, w_r, w_i)
            p_r, p_i = cmul(ar, ai, p_r, p_i)
            zcat_v[here, :lanes] = (zr_v[b, here, :] + w_r).astype(BF16)
            zcat_v[here, lanes:] = (zi_v[b, here, :] + w_i).astype(BF16)
            wcat_v[b, here, :lanes] = p_r.astype(BF16)
            wcat_v[b, here, lanes:] = p_i.astype(BF16)
        gains_r, gains_i = [], []
        for g in range(b * gpb, (b + 1) * gpb):
            g_r, g_i = cmul(cr_v[g], ci_v[g], f_r[g:g + 1], f_i[g:g + 1])
            gains_r.append(g_r)
            gains_i.append(g_i)

        m_r = diagonal(jnp.concatenate(gains_r, axis=0))
        m_i = diagonal(jnp.concatenate(gains_i, axis=0))
        crm_v[b], cim_v[b] = m_r, m_i
        mats = jnp.concatenate([m_r.astype(BF16), (-m_i).astype(BF16)], axis=1)
        col = pl.ds(b * 128, 128)
        resp_v[:, col] = nt_dot(zcat_v[...], mats) + sk_v[:, col] * xp_v[:, col].astype(F32)

    A_r, A_i = a_all_v[:blocks], a_all_v[blocks:]
    zero = jnp.zeros((blocks, lanes), F32)

    def horner(d, h):
        pltpu.make_async_remote_copy(
            src_ref=msg_v, dst_ref=recv_v.at[d], send_sem=send_sem.at[d], recv_sem=recv_sem.at[d],
            device_id=(d, core), device_id_type=MESH).wait_recv()
        got = recv_v[d].astype(F32)
        n_r, n_i = cmul(A_r, A_i, h[0], h[1])
        return n_r + got[:blocks], n_i + got[blocks:]

    h_r, h_i = lax.fori_loop(0, me, horner, (zero, zero))
    h_v[:blocks] = h_r
    h_v[blocks:] = h_i

    for b in range(blocks):
        k_r, k_i = cmul(crm_v[b], cim_v[b], h_v[b:b + 1], h_v[blocks + b:blocks + b + 1])
        mats = jnp.concatenate([k_r.astype(BF16), (-k_i).astype(BF16)], axis=1)
        col = pl.ds(b * 128, 128)
        total = resp_v[:, col] + nt_dot(wcat_v[b], mats)
        act_v[:, col] = jax.nn.gelu(total).astype(BF16)

    back = jnp.where(r1 == (r0 % length) * chunks + r0 // length, 1.0, 0.0).astype(BF16)
    act = jnp.dot(back, act_v[...], preferred_element_type=F32).astype(BF16)

    for c in copies[9:]:
        c.wait()
    piece = inbox_v.shape[-1]
    pieces = width // piece

    def exchange(j, k):
        to = lax.rem(core + k, ntp)
        return pltpu.make_async_remote_copy(
            src_ref=part_v.at[j, to], dst_ref=inbox_v.at[j, k - 1],
            send_sem=psend_sem.at[j, k - 1], recv_sem=precv_sem.at[j, k - 1],
            device_id=(me, to), device_id_type=MESH)

    for j in range(pieces):
        col = pl.ds(j * piece, piece)
        for which, weight in enumerate((vw_v, gw_v)):
            part = jnp.dot(act, weight[:, col], preferred_element_type=F32).astype(BF16)
            for i in range(ntp):
                part_v[j, i, which] = part[i * own_rows:(i + 1) * own_rows]
        for k in range(1, ntp):
            exchange(j, k).start()
    for j in range(pieces):
        col = pl.ds(j * piece, piece)
        for k in range(1, ntp):
            exchange(j, k).wait_recv()
        sums = []
        for which, bias in enumerate((vb_v, gb_v)):
            total = part_v[j, core, which].astype(F32)
            for k in range(1, ntp):
                total = total + inbox_v[j, k - 1, which].astype(F32)
            sums.append(total + bias[:, col])
        out_ref[:, col] = (sums[0] * jax.nn.sigmoid(sums[1])).astype(BF16)
    for j in range(pieces):
        for k in range(1, ntp):
            exchange(j, k).wait_send()

    @pl.loop(me + 1, nsp)
    def _(d):
        outgoing(nsp + me - d).wait_send()


def local(nsp, ntp, features, lambda_real, lambda_imag, log_step, input_real, input_imag, real_output,
          imaginary_output, skip_gain, value_weight, gate_weight, value_bias, gate_bias):
    rows, channels = features.shape
    groups, state = lambda_real.shape
    size = input_real.shape[2]
    input_real, input_imag = jnp.swapaxes(input_real, 1, 2), jnp.swapaxes(input_imag, 1, 2)
    width = value_weight.shape[1]
    gpb = 128 // size
    lanes, blocks, chunks = gpb * state, groups // gpb, 16
    piece = min(512, width)
    args = (features, lambda_real, lambda_imag, log_step[None], input_real, input_imag, real_output,
            imaginary_output, skip_gain[None], value_weight, gate_weight, value_bias[None], gate_bias[None])
    scratch = [pltpu.VMEM(a.shape, a.dtype) for a in args]
    scratch += [
        pltpu.VMEM((rows, channels), BF16),
        pltpu.VMEM((blocks, rows, lanes), F32),
        pltpu.VMEM((blocks, rows, lanes), F32),
        pltpu.VMEM((rows, 2 * lanes), BF16),
        pltpu.VMEM((blocks, rows, 2 * lanes), BF16),
        pltpu.VMEM((blocks, 128, lanes), F32),
        pltpu.VMEM((blocks, 128, lanes), F32),
        pltpu.VMEM((rows, channels), F32),
        pltpu.VMEM((rows, channels), BF16),
        pltpu.VMEM((4, blocks, chunks, lanes), F32),
        pltpu.VMEM((2 * blocks, lanes), F32),
        pltpu.VMEM((2 * blocks, lanes), F32),
        pltpu.VMEM((2 * blocks, lanes), BF16),
        pltpu.VMEM((nsp, 2 * blocks, lanes), BF16),
        pltpu.VMEM((2 * blocks, lanes), F32),
        pltpu.VMEM((width // piece, ntp, 2, rows // ntp, piece), BF16),
        pltpu.VMEM((width // piece, ntp - 1, 2, rows // ntp, piece), BF16),
        pltpu.SemaphoreType.DMA((len(args),)),
        pltpu.SemaphoreType.DMA((nsp,)),
        pltpu.SemaphoreType.DMA((nsp,)),
        pltpu.SemaphoreType.DMA((width // piece, ntp - 1)),
        pltpu.SemaphoreType.DMA((width // piece, ntp - 1)),
    ]
    return pl.pallas_call(
        functools.partial(kernel, nsp, ntp, (rows, groups, state, size, width)),
        out_shape=jax.ShapeDtypeStruct((rows // ntp, width), BF16),
        in_specs=[pl.BlockSpec(memory_space=pl.ANY)] * len(args),
        out_specs=pl.BlockSpec(memory_space=pltpu.VMEM),
        scratch_shapes=scratch,
        compiler_params=pltpu.CompilerParams(
            collective_id=0, has_side_effects=True, vmem_limit_bytes=32 * 1024 * 1024),
        name="mixer",
    )(*args)


def solution(mesh):
    in_specs = (
        P("sp", "tp"),
        P("tp", None),
        P("tp", None),
        P("tp"),
        P("tp", None, None),
        P("tp", None, None),
        P("tp", None, None),
        P("tp", None, None),
        P("tp"),
        P("tp", None),
        P("tp", None),
        P(),
        P(),
    )
    out_specs = P(("sp", "tp"), None)
    body = functools.partial(local, mesh.shape["sp"], mesh.shape["tp"])
    return jax.shard_map(body, mesh=mesh, in_specs=in_specs, out_specs=out_specs, check_vma=False)
```

```python
import functools

import jax
import jax.numpy as jnp
from jax import lax
from jax.experimental import pallas as pl
from jax.experimental.pallas import tpu as pltpu
from jax.sharding import PartitionSpec as P

MESH = pl.DeviceIdType.MESH
F32 = jnp.float32
BF16 = jnp.bfloat16


def iota(shape, dim):
    return lax.broadcasted_iota(jnp.int32, shape, dim)


def cmul(ar, ai, br, bi):
    return ar * br - ai * bi, ar * bi + ai * br


def nt_dot(left, right):
    return lax.dot_general(left, right, (((1,), (1,)), ((), ())), preferred_element_type=F32)


def kernel(nsp, ntp, dims, *refs):
    rows, groups, state, size, width = dims
    (x_h, lr_h, li_h, ls_h, br_h, bi_h, cr_h, ci_h, sk_h, vw_h, gw_h, vb_h, gb_h, out_ref,
     x_v, lr_v, li_v, ls_v, br_v, bi_v, cr_v, ci_v, sk_v, vw_v, gw_v, vb_v, gb_v,
     xp_v, zr_v, zi_v, zcat_v, wcat_v, crm_v, cim_v, resp_v, act_v,
     hx_v, fin_v, a_all_v, msg_v, recv_v, h_v, part_v, inbox_v,
     in_sem, send_sem, recv_sem, psend_sem, precv_sem) = refs
    me = lax.axis_index("sp")
    core = lax.axis_index("tp")
    gpb = 128 // size
    lanes = gpb * state
    blocks = groups // gpb
    chunks = 16
    length = rows // chunks
    own_rows = rows // ntp

    hbm = (ls_h, lr_h, li_h, x_h, br_h, bi_h, cr_h, ci_h, sk_h, vb_h, gb_h, vw_h, gw_h)
    vmem = (ls_v, lr_v, li_v, x_v, br_v, bi_v, cr_v, ci_v, sk_v, vb_v, gb_v, vw_v, gw_v)
    copies = [pltpu.make_async_copy(s, d, in_sem.at[i]) for i, (s, d) in enumerate(zip(hbm, vmem))]
    for c in copies:
        c.start()

    barrier = pltpu.get_barrier_semaphore()
    for k in range(1, ntp):
        pl.semaphore_signal(barrier, inc=1, device_id=(me, lax.rem(core + k, ntp)), device_id_type=MESH)

    @pl.loop(1, nsp)
    def _(k):
        pl.semaphore_signal(barrier, inc=1, device_id=(lax.rem(me + k, nsp), core), device_id_type=MESH)

    for c in copies[:3]:
        c.wait()
    eye = iota((groups, groups), 0) == iota((groups, groups), 1)
    step = jnp.exp(jnp.sum(jnp.where(eye, ls_v[...], 0.0), axis=1, keepdims=True))
    lam_r, lam_i = lr_v[...], li_v[...]
    mag = jnp.exp(lam_r * step)
    phase = lam_i * step
    t_r, t_i = mag * jnp.cos(phase), mag * jnp.sin(phase)
    den = lam_r * lam_r + lam_i * lam_i
    n_r = t_r - 1.0
    f_r = (n_r * lam_r + t_i * lam_i) / den
    f_i = (t_i * lam_r - n_r * lam_i) / den

    per = 128 // state
    row8, lane8 = iota((gpb, 128), 0), iota((gpb, 128), 1)

    def flat(value, b):
        sub = value[b * gpb:(b + 1) * gpb]
        dup = jnp.concatenate([sub] * per, axis=1)
        return jnp.concatenate(
            [jnp.sum(jnp.where(row8 == per * j + lane8 // state, dup, 0.0), axis=0, keepdims=True)
             for j in range(gpb // per)], axis=1)

    r0, r1 = iota((rows, rows), 0), iota((rows, rows), 1)
    shuffle = jnp.where(r1 == (r0 % chunks) * length + r0 // chunks, 1.0, 0.0).astype(BF16)
    copies[3].wait()
    xp_v[...] = jnp.dot(shuffle, x_v[...], preferred_element_type=F32).astype(BF16)


    c_mask = iota((128, lanes), 0) // size == iota((128, lanes), 1) // state

    def diagonal(tall):
        return jnp.where(c_mask, jnp.concatenate([tall] * gpb, axis=1), 0.0)

    copies[4].wait()
    copies[5].wait()
    crow = iota((chunks, lanes), 0)

    def shift(value, s):
        return jnp.where(crow >= s, pltpu.roll(value, s, 0), 0.0)

    for b in range(blocks):
        xb = xp_v[:, b * 128:(b + 1) * 128]

        def inject(ref):
            mat = diagonal(ref[b * gpb:(b + 1) * gpb].reshape(128, state)).astype(BF16)
            return jnp.dot(xb, mat, preferred_element_type=F32)

        zr_v[b] = inject(br_v)
        zi_v[b] = inject(bi_v)
        a1r, a1i = flat(t_r, b), flat(t_i, b)
        ar, ai = jnp.broadcast_to(a1r, (chunks, lanes)), jnp.broadcast_to(a1i, (chunks, lanes))
        z_r = z_i = None
        for o in range(length):
            here = pl.ds(o * chunks, chunks)
            if o == 0:
                z_r, z_i = zr_v[b, here, :], zi_v[b, here, :]
            else:
                p_r, p_i = cmul(ar, ai, z_r, z_i)
                z_r, z_i = p_r + zr_v[b, here, :], p_i + zi_v[b, here, :]
                zr_v[b, here, :] = z_r
                zi_v[b, here, :] = z_i
        qr, qi = ar, ai
        s = 1
        while s < length:
            qr, qi = cmul(qr, qi, qr, qi)
            s *= 2
        pw_r, pw_i = jnp.ones_like(qr), jnp.zeros_like(qr)
        s = 1
        while s < chunks:
            m_r, m_i = cmul(qr, qi, shift(z_r, s), shift(z_i, s))
            z_r, z_i = z_r + m_r, z_i + m_i
            bit = (crow // s) % 2 == 1
            pw_r, pw_i = cmul(pw_r, pw_i, jnp.where(bit, qr, 1.0), jnp.where(bit, qi, 0.0))
            qr, qi = cmul(qr, qi, qr, qi)
            s *= 2
        hx_v[0, b], hx_v[1, b] = shift(z_r, 1), shift(z_i, 1)
        fin_v[b:b + 1] = z_r[chunks - 1:]
        fin_v[blocks + b:blocks + b + 1] = z_i[chunks - 1:]
        a_all_v[b:b + 1] = qr[:1]
        a_all_v[blocks + b:blocks + b + 1] = qi[:1]
        hx_v[2, b], hx_v[3, b] = pw_r, pw_i
    msg_v[...] = fin_v[...].astype(BF16)

    pl.semaphore_wait(barrier, nsp - 1 + ntp - 1)

    def outgoing(d):
        return pltpu.make_async_remote_copy(
            src_ref=msg_v, dst_ref=recv_v.at[me], send_sem=send_sem.at[d], recv_sem=recv_sem.at[me],
            device_id=(d, core), device_id_type=MESH)

    @pl.loop(me + 1, nsp)
    def _(d):
        outgoing(nsp + me - d).start()

    copies[6].wait()
    copies[7].wait()
    copies[8].wait()
    for b in range(blocks):
        a1r, a1i = flat(t_r, b), flat(t_i, b)
        ar, ai = jnp.broadcast_to(a1r, (chunks, lanes)), jnp.broadcast_to(a1i, (chunks, lanes))
        w_r, w_i = hx_v[0, b], hx_v[1, b]
        p_r, p_i = hx_v[2, b], hx_v[3, b]
        for o in range(length):
            here = pl.ds(o * chunks, chunks)
            w_r, w_i = cmul(ar, ai, w_r, w_i)
            p_r, p_i = cmul(ar, ai, p_r, p_i)
            zcat_v[here, :lanes] = (zr_v[b, here, :] + w_r).astype(BF16)
            zcat_v[here, lanes:] = (zi_v[b, here, :] + w_i).astype(BF16)
            wcat_v[b, here, :lanes] = p_r.astype(BF16)
            wcat_v[b, here, lanes:] = p_i.astype(BF16)
        gains_r, gains_i = [], []
        for g in range(b * gpb, (b + 1) * gpb):
            g_r, g_i = cmul(cr_v[g], ci_v[g], f_r[g:g + 1], f_i[g:g + 1])
            gains_r.append(g_r)
            gains_i.append(g_i)

        m_r = diagonal(jnp.concatenate(gains_r, axis=0))
        m_i = diagonal(jnp.concatenate(gains_i, axis=0))
        crm_v[b], cim_v[b] = m_r, m_i
        mats = jnp.concatenate([m_r.astype(BF16), (-m_i).astype(BF16)], axis=1)
        col = pl.ds(b * 128, 128)
        resp_v[:, col] = nt_dot(zcat_v[...], mats) + sk_v[:, col] * xp_v[:, col].astype(F32)

    A_r, A_i = a_all_v[:blocks], a_all_v[blocks:]
    zero = jnp.zeros((blocks, lanes), F32)

    def horner(d, h):
        pltpu.make_async_remote_copy(
            src_ref=msg_v, dst_ref=recv_v.at[d], send_sem=send_sem.at[d], recv_sem=recv_sem.at[d],
            device_id=(d, core), device_id_type=MESH).wait_recv()
        got = recv_v[d].astype(F32)
        n_r, n_i = cmul(A_r, A_i, h[0], h[1])
        return n_r + got[:blocks], n_i + got[blocks:]

    h_r, h_i = lax.fori_loop(0, me, horner, (zero, zero))
    h_v[:blocks] = h_r
    h_v[blocks:] = h_i

    for b in range(blocks):
        k_r, k_i = cmul(crm_v[b], cim_v[b], h_v[b:b + 1], h_v[blocks + b:blocks + b + 1])
        mats = jnp.concatenate([k_r.astype(BF16), (-k_i).astype(BF16)], axis=1)
        col = pl.ds(b * 128, 128)
        total = resp_v[:, col] + nt_dot(wcat_v[b], mats)
        act_v[:, col] = jax.nn.gelu(total).astype(BF16)

    back = jnp.where(r1 == (r0 % length) * chunks + r0 // length, 1.0, 0.0).astype(BF16)
    act = jnp.dot(back, act_v[...], preferred_element_type=F32).astype(BF16)

    for c in copies[9:]:
        c.wait()
    piece = inbox_v.shape[-1]
    pieces = width // piece

    def exchange(j, k):
        to = lax.rem(core + k, ntp)
        return pltpu.make_async_remote_copy(
            src_ref=part_v.at[j, to], dst_ref=inbox_v.at[j, k - 1],
            send_sem=psend_sem.at[j, k - 1], recv_sem=precv_sem.at[j, k - 1],
            device_id=(me, to), device_id_type=MESH)

    for j in range(pieces):
        col = pl.ds(j * piece, piece)
        for which, weight in enumerate((vw_v, gw_v)):
            part = jnp.dot(act, weight[:, col], preferred_element_type=F32).astype(BF16)
            for i in range(ntp):
                part_v[j, i, which] = part[i * own_rows:(i + 1) * own_rows]
        for k in range(1, ntp):
            exchange(j, k).start()
    for j in range(pieces):
        col = pl.ds(j * piece, piece)
        for k in range(1, ntp):
            exchange(j, k).wait_recv()
        sums = []
        for which, bias in enumerate((vb_v, gb_v)):
            total = part_v[j, core, which].astype(F32)
            for k in range(1, ntp):
                total = total + inbox_v[j, k - 1, which].astype(F32)
            sums.append(total + bias[:, col])
        out_ref[:, col] = (sums[0] * jax.nn.sigmoid(sums[1])).astype(BF16)
    for j in range(pieces):
        for k in range(1, ntp):
            exchange(j, k).wait_send()

    @pl.loop(me + 1, nsp)
    def _(d):
        outgoing(nsp + me - d).wait_send()


def local(nsp, ntp, features, lambda_real, lambda_imag, log_step, input_real, input_imag, real_output,
          imaginary_output, skip_gain, value_weight, gate_weight, value_bias, gate_bias):
    rows, channels = features.shape
    groups, state = lambda_real.shape
    size = input_real.shape[2]
    input_real, input_imag = jnp.swapaxes(input_real, 1, 2), jnp.swapaxes(input_imag, 1, 2)
    width = value_weight.shape[1]
    gpb = 128 // size
    lanes, blocks, chunks = gpb * state, groups // gpb, 16
    piece = min(512, width)
    args = (features, lambda_real, lambda_imag, log_step[None], input_real, input_imag, real_output,
            imaginary_output, skip_gain[None], value_weight, gate_weight, value_bias[None], gate_bias[None])
    scratch = [pltpu.VMEM(a.shape, a.dtype) for a in args]
    scratch += [
        pltpu.VMEM((rows, channels), BF16),
        pltpu.VMEM((blocks, rows, lanes), F32),
        pltpu.VMEM((blocks, rows, lanes), F32),
        pltpu.VMEM((rows, 2 * lanes), BF16),
        pltpu.VMEM((blocks, rows, 2 * lanes), BF16),
        pltpu.VMEM((blocks, 128, lanes), F32),
        pltpu.VMEM((blocks, 128, lanes), F32),
        pltpu.VMEM((rows, channels), F32),
        pltpu.VMEM((rows, channels), BF16),
        pltpu.VMEM((4, blocks, chunks, lanes), F32),
        pltpu.VMEM((2 * blocks, lanes), F32),
        pltpu.VMEM((2 * blocks, lanes), F32),
        pltpu.VMEM((2 * blocks, lanes), BF16),
        pltpu.VMEM((nsp, 2 * blocks, lanes), BF16),
        pltpu.VMEM((2 * blocks, lanes), F32),
        pltpu.VMEM((width // piece, ntp, 2, rows // ntp, piece), BF16),
        pltpu.VMEM((width // piece, ntp - 1, 2, rows // ntp, piece), BF16),
        pltpu.SemaphoreType.DMA((len(args),)),
        pltpu.SemaphoreType.DMA((nsp,)),
        pltpu.SemaphoreType.DMA((nsp,)),
        pltpu.SemaphoreType.DMA((width // piece, ntp - 1)),
        pltpu.SemaphoreType.DMA((width // piece, ntp - 1)),
    ]
    return pl.pallas_call(
        functools.partial(kernel, nsp, ntp, (rows, groups, state, size, width)),
        out_shape=pltpu.VMEM((rows // ntp, width), BF16),
        in_specs=[pl.BlockSpec(memory_space=pl.ANY)] * len(args),
        out_specs=pl.BlockSpec(memory_space=pltpu.VMEM),
        scratch_shapes=scratch,
        compiler_params=pltpu.CompilerParams(
            collective_id=0, has_side_effects=True, vmem_limit_bytes=60 * 1024 * 1024),
        name="mixer",
    )(*args)


def solution(mesh):
    in_specs = (
        P("sp", "tp"),
        P("tp", None),
        P("tp", None),
        P("tp"),
        P("tp", None, None),
        P("tp", None, None),
        P("tp", None, None),
        P("tp", None, None),
        P("tp"),
        P("tp", None),
        P("tp", None),
        P(),
        P(),
    )
    out_specs = P(("sp", "tp"), None)
    body = functools.partial(local, mesh.shape["sp"], mesh.shape["tp"])
    return jax.shard_map(body, mesh=mesh, in_specs=in_specs, out_specs=out_specs, check_vma=False)
```

```python
import functools

import jax
import jax.numpy as jnp
from jax import lax
from jax.experimental import pallas as pl
from jax.experimental.pallas import tpu as pltpu
from jax.sharding import PartitionSpec as P

MESH = pl.DeviceIdType.MESH
F32 = jnp.float32
BF16 = jnp.bfloat16


def iota(shape, dim):
    return lax.broadcasted_iota(jnp.int32, shape, dim)


def cmul(ar, ai, br, bi):
    return ar * br - ai * bi, ar * bi + ai * br


def nt_dot(left, right):
    return lax.dot_general(left, right, (((1,), (1,)), ((), ())), preferred_element_type=F32)


def kernel(nsp, ntp, dims, *refs):
    rows, groups, state, size, width = dims
    (x_h, lr_h, li_h, ls_h, br_h, bi_h, cr_h, ci_h, sk_h, vw_h, gw_h, vb_h, gb_h, out_ref,
     x_v, lr_v, li_v, ls_v, br_v, bi_v, cr_v, ci_v, sk_v, vw_v, gw_v, vb_v, gb_v,
     xp_v, zr_v, zi_v, zcat_v, wcat_v, crm_v, cim_v, resp_v, act_v,
     hx_v, fin_v, a_all_v, msg_v, recv_v, h_v, part_v, inbox_v,
     in_sem, send_sem, recv_sem, psend_sem, precv_sem) = refs
    me = lax.axis_index("sp")
    core = lax.axis_index("tp")
    gpb = 128 // size
    lanes = gpb * state
    blocks = groups // gpb
    chunks = 16
    length = rows // chunks
    own_rows = rows // ntp

    hbm = (ls_h, lr_h, li_h, x_h, br_h, bi_h, cr_h, ci_h, sk_h, vb_h, gb_h, vw_h, gw_h)
    vmem = (ls_v, lr_v, li_v, x_v, br_v, bi_v, cr_v, ci_v, sk_v, vb_v, gb_v, vw_v, gw_v)
    copies = [pltpu.make_async_copy(s, d, in_sem.at[i]) for i, (s, d) in enumerate(zip(hbm, vmem))]
    for c in copies[:6]:
        c.start()

    barrier = pltpu.get_barrier_semaphore()
    for k in range(1, ntp):
        pl.semaphore_signal(barrier, inc=1, device_id=(me, lax.rem(core + k, ntp)), device_id_type=MESH)

    @pl.loop(1, nsp)
    def _(k):
        pl.semaphore_signal(barrier, inc=1, device_id=(lax.rem(me + k, nsp), core), device_id_type=MESH)

    for c in copies[:3]:
        c.wait()
    eye = iota((groups, groups), 0) == iota((groups, groups), 1)
    step = jnp.exp(jnp.sum(jnp.where(eye, ls_v[...], 0.0), axis=1, keepdims=True))
    lam_r, lam_i = lr_v[...], li_v[...]
    mag = jnp.exp(lam_r * step)
    phase = lam_i * step
    t_r, t_i = mag * jnp.cos(phase), mag * jnp.sin(phase)
    den = lam_r * lam_r + lam_i * lam_i
    n_r = t_r - 1.0
    f_r = (n_r * lam_r + t_i * lam_i) / den
    f_i = (t_i * lam_r - n_r * lam_i) / den

    per = 128 // state
    row8, lane8 = iota((gpb, 128), 0), iota((gpb, 128), 1)

    def flat(value, b):
        sub = value[b * gpb:(b + 1) * gpb]
        dup = jnp.concatenate([sub] * per, axis=1)
        return jnp.concatenate(
            [jnp.sum(jnp.where(row8 == per * j + lane8 // state, dup, 0.0), axis=0, keepdims=True)
             for j in range(gpb // per)], axis=1)

    r0, r1 = iota((rows, rows), 0), iota((rows, rows), 1)
    shuffle = jnp.where(r1 == (r0 % chunks) * length + r0 // chunks, 1.0, 0.0).astype(BF16)
    copies[3].wait()
    xp_v[...] = jnp.dot(shuffle, x_v[...], preferred_element_type=F32).astype(BF16)


    c_mask = iota((128, lanes), 0) // size == iota((128, lanes), 1) // state

    def diagonal(tall):
        return jnp.where(c_mask, jnp.concatenate([tall] * gpb, axis=1), 0.0)

    copies[4].wait()
    copies[5].wait()
    for c in copies[6:]:
        c.start()
    crow = iota((chunks, lanes), 0)

    def shift(value, s):
        return jnp.where(crow >= s, pltpu.roll(value, s, 0), 0.0)

    for b in range(blocks):
        xb = xp_v[:, b * 128:(b + 1) * 128]

        def inject(ref):
            mat = diagonal(ref[b * gpb:(b + 1) * gpb].reshape(128, state)).astype(BF16)
            return jnp.dot(xb, mat, preferred_element_type=F32)

        zr_v[b] = inject(br_v)
        zi_v[b] = inject(bi_v)
        a1r, a1i = flat(t_r, b), flat(t_i, b)
        ar, ai = jnp.broadcast_to(a1r, (chunks, lanes)), jnp.broadcast_to(a1i, (chunks, lanes))
        z_r = z_i = None
        for o in range(length):
            here = pl.ds(o * chunks, chunks)
            if o == 0:
                z_r, z_i = zr_v[b, here, :], zi_v[b, here, :]
            else:
                p_r, p_i = cmul(ar, ai, z_r, z_i)
                z_r, z_i = p_r + zr_v[b, here, :], p_i + zi_v[b, here, :]
                zr_v[b, here, :] = z_r
                zi_v[b, here, :] = z_i
        qr, qi = ar, ai
        s = 1
        while s < length:
            qr, qi = cmul(qr, qi, qr, qi)
            s *= 2
        pw_r, pw_i = jnp.ones_like(qr), jnp.zeros_like(qr)
        s = 1
        while s < chunks:
            m_r, m_i = cmul(qr, qi, shift(z_r, s), shift(z_i, s))
            z_r, z_i = z_r + m_r, z_i + m_i
            bit = (crow // s) % 2 == 1
            pw_r, pw_i = cmul(pw_r, pw_i, jnp.where(bit, qr, 1.0), jnp.where(bit, qi, 0.0))
            qr, qi = cmul(qr, qi, qr, qi)
            s *= 2
        hx_v[0, b], hx_v[1, b] = shift(z_r, 1), shift(z_i, 1)
        fin_v[b:b + 1] = z_r[chunks - 1:]
        fin_v[blocks + b:blocks + b + 1] = z_i[chunks - 1:]
        a_all_v[b:b + 1] = qr[:1]
        a_all_v[blocks + b:blocks + b + 1] = qi[:1]
        hx_v[2, b], hx_v[3, b] = pw_r, pw_i
    msg_v[...] = fin_v[...].astype(BF16)

    pl.semaphore_wait(barrier, nsp - 1 + ntp - 1)

    def outgoing(d):
        return pltpu.make_async_remote_copy(
            src_ref=msg_v, dst_ref=recv_v.at[me], send_sem=send_sem.at[d], recv_sem=recv_sem.at[me],
            device_id=(d, core), device_id_type=MESH)

    @pl.loop(me + 1, nsp)
    def _(d):
        outgoing(d).start()

    copies[6].wait()
    copies[7].wait()
    copies[8].wait()
    for b in range(blocks):
        a1r, a1i = flat(t_r, b), flat(t_i, b)
        ar, ai = jnp.broadcast_to(a1r, (chunks, lanes)), jnp.broadcast_to(a1i, (chunks, lanes))
        w_r, w_i = hx_v[0, b], hx_v[1, b]
        p_r, p_i = hx_v[2, b], hx_v[3, b]
        for o in range(length):
            here = pl.ds(o * chunks, chunks)
            w_r, w_i = cmul(ar, ai, w_r, w_i)
            p_r, p_i = cmul(ar, ai, p_r, p_i)
            zcat_v[here, :lanes] = (zr_v[b, here, :] + w_r).astype(BF16)
            zcat_v[here, lanes:] = (zi_v[b, here, :] + w_i).astype(BF16)
            wcat_v[b, here, :lanes] = p_r.astype(BF16)
            wcat_v[b, here, lanes:] = p_i.astype(BF16)
        gains_r, gains_i = [], []
        for g in range(b * gpb, (b + 1) * gpb):
            g_r, g_i = cmul(cr_v[g], ci_v[g], f_r[g:g + 1], f_i[g:g + 1])
            gains_r.append(g_r)
            gains_i.append(g_i)

        m_r = diagonal(jnp.concatenate(gains_r, axis=0))
        m_i = diagonal(jnp.concatenate(gains_i, axis=0))
        crm_v[b], cim_v[b] = m_r, m_i
        mats = jnp.concatenate([m_r.astype(BF16), (-m_i).astype(BF16)], axis=1)
        col = pl.ds(b * 128, 128)
        resp_v[:, col] = nt_dot(zcat_v[...], mats) + sk_v[:, col] * xp_v[:, col].astype(F32)

    A_r, A_i = a_all_v[:blocks], a_all_v[blocks:]
    zero = jnp.zeros((blocks, lanes), F32)

    def gather(k, carry):
        h_r, h_i, p_r, p_i = carry
        d = me - 1 - k
        pltpu.make_async_remote_copy(
            src_ref=msg_v, dst_ref=recv_v.at[d], send_sem=send_sem.at[d], recv_sem=recv_sem.at[d],
            device_id=(d, core), device_id_type=MESH).wait_recv()
        got = recv_v[d].astype(F32)
        m_r, m_i = cmul(p_r, p_i, got[:blocks], got[blocks:])
        return (h_r + m_r, h_i + m_i) + cmul(p_r, p_i, A_r, A_i)

    h_r, h_i, _, _ = lax.fori_loop(0, me, gather, (zero, zero, zero + 1.0, zero))
    h_v[:blocks] = h_r
    h_v[blocks:] = h_i

    for b in range(blocks):
        k_r, k_i = cmul(crm_v[b], cim_v[b], h_v[b:b + 1], h_v[blocks + b:blocks + b + 1])
        mats = jnp.concatenate([k_r.astype(BF16), (-k_i).astype(BF16)], axis=1)
        col = pl.ds(b * 128, 128)
        total = resp_v[:, col] + nt_dot(wcat_v[b], mats)
        act_v[:, col] = jax.nn.gelu(total).astype(BF16)

    back = jnp.where(r1 == (r0 % length) * chunks + r0 // length, 1.0, 0.0).astype(BF16)
    act = jnp.dot(back, act_v[...], preferred_element_type=F32).astype(BF16)

    for c in copies[9:]:
        c.wait()
    piece = inbox_v.shape[-1]
    pieces = width // piece

    def exchange(j, k):
        to = lax.rem(core + k, ntp)
        return pltpu.make_async_remote_copy(
            src_ref=part_v.at[j, to], dst_ref=inbox_v.at[j, k - 1],
            send_sem=psend_sem.at[j, k - 1], recv_sem=precv_sem.at[j, k - 1],
            device_id=(me, to), device_id_type=MESH)

    for j in range(pieces):
        col = pl.ds(j * piece, piece)
        for which, weight in enumerate((vw_v, gw_v)):
            part = jnp.dot(act, weight[:, col], preferred_element_type=F32).astype(BF16)
            for i in range(ntp):
                part_v[j, i, which] = part[i * own_rows:(i + 1) * own_rows]
        for k in range(1, ntp):
            exchange(j, k).start()
    for j in range(pieces):
        col = pl.ds(j * piece, piece)
        for k in range(1, ntp):
            exchange(j, k).wait_recv()
        sums = []
        for which, bias in enumerate((vb_v, gb_v)):
            total = part_v[j, core, which].astype(F32)
            for k in range(1, ntp):
                total = total + inbox_v[j, k - 1, which].astype(F32)
            sums.append(total + bias[:, col])
        out_ref[:, col] = (sums[0] * jax.nn.sigmoid(sums[1])).astype(BF16)
    for j in range(pieces):
        for k in range(1, ntp):
            exchange(j, k).wait_send()

    @pl.loop(me + 1, nsp)
    def _(d):
        outgoing(d).wait_send()


def local(nsp, ntp, features, lambda_real, lambda_imag, log_step, input_real, input_imag, real_output,
          imaginary_output, skip_gain, value_weight, gate_weight, value_bias, gate_bias):
    rows, channels = features.shape
    groups, state = lambda_real.shape
    size = input_real.shape[2]
    input_real, input_imag = jnp.swapaxes(input_real, 1, 2), jnp.swapaxes(input_imag, 1, 2)
    width = value_weight.shape[1]
    gpb = 128 // size
    lanes, blocks, chunks = gpb * state, groups // gpb, 16
    piece = min(512, width)
    args = (features, lambda_real, lambda_imag, log_step[None], input_real, input_imag, real_output,
            imaginary_output, skip_gain[None], value_weight, gate_weight, value_bias[None], gate_bias[None])
    scratch = [pltpu.VMEM(a.shape, a.dtype) for a in args]
    scratch += [
        pltpu.VMEM((rows, channels), BF16),
        pltpu.VMEM((blocks, rows, lanes), F32),
        pltpu.VMEM((blocks, rows, lanes), F32),
        pltpu.VMEM((rows, 2 * lanes), BF16),
        pltpu.VMEM((blocks, rows, 2 * lanes), BF16),
        pltpu.VMEM((blocks, 128, lanes), F32),
        pltpu.VMEM((blocks, 128, lanes), F32),
        pltpu.VMEM((rows, channels), F32),
        pltpu.VMEM((rows, channels), BF16),
        pltpu.VMEM((4, blocks, chunks, lanes), F32),
        pltpu.VMEM((2 * blocks, lanes), F32),
        pltpu.VMEM((2 * blocks, lanes), F32),
        pltpu.VMEM((2 * blocks, lanes), BF16),
        pltpu.VMEM((nsp, 2 * blocks, lanes), BF16),
        pltpu.VMEM((2 * blocks, lanes), F32),
        pltpu.VMEM((width // piece, ntp, 2, rows // ntp, piece), BF16),
        pltpu.VMEM((width // piece, ntp - 1, 2, rows // ntp, piece), BF16),
        pltpu.SemaphoreType.DMA((len(args),)),
        pltpu.SemaphoreType.DMA((nsp,)),
        pltpu.SemaphoreType.DMA((nsp,)),
        pltpu.SemaphoreType.DMA((width // piece, ntp - 1)),
        pltpu.SemaphoreType.DMA((width // piece, ntp - 1)),
    ]
    return pl.pallas_call(
        functools.partial(kernel, nsp, ntp, (rows, groups, state, size, width)),
        out_shape=pltpu.VMEM((rows // ntp, width), BF16),
        in_specs=[pl.BlockSpec(memory_space=pl.ANY)] * len(args),
        out_specs=pl.BlockSpec(memory_space=pltpu.VMEM),
        scratch_shapes=scratch,
        compiler_params=pltpu.CompilerParams(
            collective_id=0, has_side_effects=True, vmem_limit_bytes=60 * 1024 * 1024),
        name="mixer",
    )(*args)


def solution(mesh):
    in_specs = (
        P("sp", "tp"),
        P("tp", None),
        P("tp", None),
        P("tp"),
        P("tp", None, None),
        P("tp", None, None),
        P("tp", None, None),
        P("tp", None, None),
        P("tp"),
        P("tp", None),
        P("tp", None),
        P(),
        P(),
    )
    out_specs = P(("sp", "tp"), None)
    body = functools.partial(local, mesh.shape["sp"], mesh.shape["tp"])
    return jax.shard_map(body, mesh=mesh, in_specs=in_specs, out_specs=out_specs, check_vma=False)
```
